32 devices in a mesh: ep: 4 (over y, x), tp: 8 (over z, core).
Axes of the slice: x: 2, y: 2, z: 4, core: 2. Of those that a mesh axis runs over, the one named last changes fastest.
Arguments:
- features: bfloat16 [64, 1024], P('ep', 'tp'), may hold values from -6 to 6
- key_table: bfloat16 [65536, 1024], P('ep', 'tp'), may hold values from -0.1875 to 0.1875
- value_table: bfloat16 [65536, 1024], P('ep', 'tp'), may hold values from -6 to 6
- chosen: int32 [64, 4, 16], P('ep'), may hold values from 0 to 65535
- scores: float32 [64, 4, 16], P('ep'), may hold values from -8 to 8
Outputs:
- mixed: bfloat16 [64, 1024], P('ep', 'tp')
The draws below stay inside these ranges and needn't reach their ends.
Inputs may be any that keep to these rules, and one draw needn't show every extreme that they name: Every chosen row is a row of the tables, 0 to 65535; rows may repeat, and a few rows are far more popular than the rest.
All inputs are finite; a program needn't handle non-finite values.
Results may differ from the reference program's by a relative error of at most 0.0065.
Values may be sent and summed in bfloat16 or wider, within the bound.
A program may use at most 64 MiB of HBM per device.

```python
import math
import jax
import jax.numpy as jnp
import numpy as np
from jax import lax

D = 1024
HEADS = 4
TOPK = 16
TOK_DEV = 16
TOKENS = 64
EXPERTS = 65536


def plant(result, rng, low, largest):
    index_at = [jax.random.randint(jax.random.fold_in(rng, axis), (), 0, length) for axis, length in enumerate(result.shape)]
    main_axis = result.shape.index(max(result.shape))
    neighbour = index_at[:main_axis] + [(index_at[main_axis] + 1) % result.shape[main_axis]] + index_at[main_axis + 1:]
    return result.at[tuple(index_at)].set(low).at[tuple(neighbour)].set(largest)


def shard_levels(key, extent, cuts, least, top_value):
    def one(dim, shards_of):
        steps = jax.random.uniform(jax.random.fold_in(jax.random.fold_in(key, 6), dim), (shards_of,), jnp.float32, least / len(cuts), top_value / len(cuts))
        return jnp.repeat(jnp.exp(steps), extent[dim] // shards_of).reshape((-1,) + (1,) * (len(extent) - dim - 1))

    level = one(*cuts[0])
    for cut in cuts[1:]:
        level = level * one(*cut)
    return level


def rank_table(count, slope):
    portions = [(1 << 20) // math.isqrt(rank ** slope) + 1 for rank in range(1, count + 1)]
    spread = 1 + sum(portions) // (1 << 30)
    return np.cumsum(np.array([max(1, weight // spread) for weight in portions]))


def skewed_ids(stream_key, extent, number_of, slope):
    listing = rank_table(number_of, slope)
    pick = jax.random.randint(jax.random.fold_in(stream_key, 1), extent, 0, int(listing[number_of - 1]))
    grade = jnp.searchsorted(jnp.asarray(listing, jnp.int32), pick, side="right")
    return jax.random.permutation(jax.random.fold_in(stream_key, 2), number_of)[grade].astype(jnp.int32)


def normal_values(rng, extent, width, limit, split=(), dtype=jnp.bfloat16):
    drawn = jax.random.normal(rng, extent, jnp.float32) * width
    if len(split) > 0:
        drawn = shard_levels(rng, extent, split, -0.22, 0.18) * drawn
    return jnp.clip(drawn, min=-limit, max=limit).astype(dtype)


def setup_inputs(seed: int = 0) -> dict:
    seeds = jax.random.split(jax.random.key(seed), 6)
    return {
        "features": normal_values(seeds[0], (TOKENS, D), 1.0, 6.0, ((0, 4), (1, 8))),
        "key_table": normal_values(seeds[1], (EXPERTS, D), D ** -0.5, 0.1875, ((0, 4), (1, 8))),
        "value_table": normal_values(seeds[2], (EXPERTS, D), 1.0, 6.0, ((0, 4), (1, 8))),
        "chosen": plant(skewed_ids(seeds[3], (TOKENS, HEADS, TOPK), EXPERTS, 2), jax.random.fold_in(seeds[3], 3), 0, EXPERTS - 1).astype(jnp.int32),
        "scores": normal_values(seeds[4], (TOKENS, HEADS, TOPK), 2.0, 8.0, ((0, 4),), jnp.float32),
    }


def reference(features, key_table, value_table, chosen, scores):
    gate_weights = jax.nn.softmax(scores, axis=-1)
    block_count = TOKENS // TOK_DEV

    def per_block(block_data):
        block_tokens, block_rows, block_gates = block_data
        flat_rows = block_rows.reshape(-1).astype(jnp.int32)
        key_rows = jnp.take(key_table, flat_rows, axis=0).reshape(TOK_DEV, HEADS * TOPK, D).astype(jnp.float32)
        products = jnp.einsum("tjd,td->tj", key_rows, block_tokens.astype(jnp.float32), precision=lax.Precision.HIGHEST)
        row_weights = (block_gates.reshape(TOK_DEV, HEADS * TOPK) * jax.nn.gelu(products, approximate=False)).astype(jnp.bfloat16)
        value_rows = jnp.take(value_table, flat_rows, axis=0).reshape(TOK_DEV, HEADS * TOPK, D).astype(jnp.float32)
        summed = jnp.einsum("tj,tjd->td", row_weights.astype(jnp.float32), value_rows, precision=lax.Precision.HIGHEST)
        return summed.astype(jnp.bfloat16)

    outputs = lax.map(per_block, (features.reshape(block_count, TOK_DEV, D),
                                  chosen.reshape(block_count, TOK_DEV, HEADS, TOPK),
                                  gate_weights.reshape(block_count, TOK_DEV, HEADS, TOPK)))
    return outputs.reshape(TOKENS, D)
```

```python
import functools

import jax
import jax.numpy as jnp
from jax import lax
from jax.experimental import pallas as pl
from jax.experimental.pallas import tpu as pltpu
from jax.sharding import PartitionSpec as P

LANES = 128
GROUP = 16
MESH = pl.DeviceIdType.MESH


def matmul_nt(left, right):
    return lax.dot_general(
        left, right, (((1,), (1,)), ((), ())), preferred_element_type=jnp.float32
    )


def split_terms(value):
    upper = value.astype(jnp.bfloat16)
    lower = (value - upper.astype(jnp.float32)).astype(jnp.bfloat16)
    return upper, lower


def kernel(
    ep_size,
    tp_size,
    features_hbm,
    key_hbm,
    value_hbm,
    chosen_hbm,
    scores_hbm,
    out_ref,
    features,
    chosen,
    scores,
    key,
    value,
    dense,
    picks,
    partial,
    weights,
    summed,
    landed,
    local_sem,
    send_sem,
    recv_sem,
    tp_send,
    tp_recv,
    out_send,
    out_recv,
):
    my_ep = lax.axis_index("ep")
    my_tp = lax.axis_index("tp")
    table_rows = key.shape[0]
    blocks = table_rows // LANES
    own_tokens, heads, top = chosen_hbm.shape
    tokens = ep_size * own_tokens
    half = tokens // 2
    per_token = heads * top
    width = 2 * per_token

    def token_slot(ref, index):
        return ref.at[pl.ds(index * own_tokens, own_tokens)]

    small = (
        (features_hbm, features),
        (chosen_hbm, chosen),
        (scores_hbm, scores),
    )
    small_copies = []
    for number, (source, target) in enumerate(small):
        copy = pltpu.make_async_copy(source, token_slot(target, my_ep), local_sem.at[number])
        copy.start()
        small_copies.append(copy)
    key_copy = pltpu.make_async_copy(key_hbm, key, local_sem.at[3])
    key_copy.start()
    value_copy = pltpu.make_async_copy(value_hbm, value, local_sem.at[4])
    value_copy.start()

    barrier = pltpu.get_barrier_semaphore()
    for step in range(1, ep_size):
        pl.semaphore_signal(
            barrier, inc=1, device_id=(lax.rem(my_ep + step, ep_size), my_tp), device_id_type=MESH
        )
    for step in range(1, tp_size):
        pl.semaphore_signal(
            barrier, inc=1, device_id=(my_ep, lax.rem(my_tp + step, tp_size)), device_id_type=MESH
        )
    for copy in small_copies:
        copy.wait()
    pl.semaphore_wait(barrier, ep_size + tp_size - 2)

    def ep_copy(number, step, owner):
        target = small[number][1]
        return pltpu.make_async_remote_copy(
            src_ref=token_slot(target, owner),
            dst_ref=token_slot(target, owner),
            send_sem=send_sem.at[number, step - 1],
            recv_sem=recv_sem.at[number, step - 1],
            device_id=(lax.rem(my_ep + step, ep_size), my_tp),
            device_id_type=MESH,
        )

    def source_ep(step):
        return lax.rem(my_ep + ep_size - step, ep_size)

    for number in range(3):
        for step in range(1, ep_size):
            ep_copy(number, step, my_ep).start()

    for step in range(1, ep_size):
        ep_copy(0, step, source_ep(step)).wait_recv()
    key_copy.wait()

    token_vectors = features[...]

    def dense_step(index, carry):
        for inner in range(GROUP):
            block = index * GROUP + inner
            rows = key[pl.ds(pl.multiple_of(block * LANES, LANES), LANES), :]
            dense[pl.ds(pl.multiple_of(block * tokens, tokens), tokens), :] = matmul_nt(
                token_vectors, rows
            )
        return carry

    lax.fori_loop(0, blocks // GROUP, dense_step, 0)

    for step in range(1, ep_size):
        ep_copy(1, step, source_ep(step)).wait_recv()

    def packed(pieces):
        flat = jnp.concatenate(pieces, axis=1)
        return jnp.concatenate([flat[:half], flat[half:]], axis=1)

    picks[...] = packed([chosen[:, head, :] for head in range(heads)]) - my_ep * table_rows

    block_ids = lax.broadcasted_iota(jnp.int32, (blocks, width), 0)
    lane_ids = lax.broadcasted_iota(jnp.int32, (LANES, width), 0)
    in_first = lax.broadcasted_iota(jnp.int32, (blocks, width), 1) < per_token

    def masks(pair):
        row = picks[pl.ds(pair, 1), :]
        column_hot = jnp.where((row & (LANES - 1)) == lane_ids, 1.0, 0.0).astype(jnp.bfloat16)
        block_mask = lax.shift_right_arithmetic(row, 7) == block_ids
        return column_hot, block_mask

    def chosen_of(token, column_hot):
        upper, lower = split_terms(dense[pl.ds(token, blocks, stride=tokens), :])
        return jnp.dot(upper, column_hot, preferred_element_type=jnp.float32) + jnp.dot(
            lower, column_hot, preferred_element_type=jnp.float32
        )

    def pick_step(pair, carry):
        column_hot, block_mask = masks(pair)
        both = jnp.where(
            in_first, chosen_of(pair, column_hot), chosen_of(pair + half, column_hot)
        )
        partial[my_tp, pl.ds(pair, 1), :] = jnp.sum(
            jnp.where(block_mask, both, 0.0), axis=0, keepdims=True
        )
        return carry

    lax.fori_loop(0, half, pick_step, 0, unroll=2)

    def tp_copy(step, owner):
        return pltpu.make_async_remote_copy(
            src_ref=partial.at[owner],
            dst_ref=partial.at[owner],
            send_sem=tp_send.at[step - 1],
            recv_sem=tp_recv.at[step - 1],
            device_id=(my_ep, lax.rem(my_tp + step, tp_size)),
            device_id_type=MESH,
        )

    for step in range(1, tp_size):
        tp_copy(step, my_tp).start()

    for step in range(1, ep_size):
        ep_copy(2, step, source_ep(step)).wait_recv()
    gate_pieces = []
    for head in range(heads):
        logits = scores[:, head, :]
        powers = jnp.exp(logits - jnp.max(logits, axis=1, keepdims=True))
        gate_pieces.append(powers / jnp.sum(powers, axis=1, keepdims=True))
    gates = packed(gate_pieces)

    for step in range(1, tp_size):
        tp_copy(step, lax.rem(my_tp + tp_size - step, tp_size)).wait_recv()
    products = partial[0]
    for index in range(1, tp_size):
        products = products + partial[index]
    activated = 0.5 * products * (1.0 + lax.erf(products * (0.5**0.5)))
    weights[...] = (gates * activated).astype(jnp.bfloat16).astype(jnp.float32)

    def spread_step(pair, carry):
        column_hot, block_mask = masks(pair)
        hot = jnp.where(block_mask, weights[pl.ds(pair, 1), :], 0.0)
        for token, keep in ((pair, in_first), (pair + half, jnp.logical_not(in_first))):
            dense[pl.ds(token, blocks, stride=tokens), :] = matmul_nt(
                jnp.where(keep, hot, 0.0).astype(jnp.bfloat16), column_hot
            )
        return carry

    lax.fori_loop(0, half, spread_step, 0, unroll=2)

    value_copy.wait()

    def value_step(index, total):
        for inner in range(GROUP):
            block = index * GROUP + inner
            rows = value[pl.ds(pl.multiple_of(block * LANES, LANES), LANES), :]
            upper, lower = split_terms(
                dense[pl.ds(pl.multiple_of(block * tokens, tokens), tokens), :]
            )
            total = total + jnp.dot(upper, rows, preferred_element_type=jnp.float32)
            total = total + jnp.dot(lower, rows, preferred_element_type=jnp.float32)
        return total

    zero = jnp.zeros(summed.shape, jnp.float32)
    summed[...] = lax.fori_loop(0, blocks // GROUP, value_step, zero)

    def out_copy(step, owner):
        return pltpu.make_async_remote_copy(
            src_ref=token_slot(summed, lax.rem(my_ep + step, ep_size)),
            dst_ref=landed.at[step - 1],
            send_sem=out_send.at[step - 1],
            recv_sem=out_recv.at[step - 1],
            device_id=(lax.rem(my_ep + step, ep_size), my_tp),
            device_id_type=MESH,
        )

    for step in range(1, ep_size):
        out_copy(step, my_ep).start()
    result = summed[pl.ds(pl.multiple_of(my_ep * own_tokens, own_tokens), own_tokens), :]
    for step in range(1, ep_size):
        out_copy(step, my_ep).wait_recv()
        result = result + landed[step - 1]
    out_ref[...] = result.astype(out_ref.dtype)

    for step in range(1, ep_size):
        for number in range(3):
            ep_copy(number, step, my_ep).wait_send()
        out_copy(step, my_ep).wait_send()
    for step in range(1, tp_size):
        tp_copy(step, my_tp).wait_send()


def shards(ep_size, tp_size, features, key_table, value_table, chosen, scores):
    own_tokens, width = features.shape
    _, heads, top = chosen.shape
    table_rows = key_table.shape[0]
    tokens = ep_size * own_tokens
    packed_shape = (tokens // 2, 2 * heads * top)
    dma = pltpu.SemaphoreType.DMA
    return pl.pallas_call(
        functools.partial(kernel, ep_size, tp_size),
        out_shape=jax.ShapeDtypeStruct((own_tokens, width), jnp.bfloat16),
        in_specs=[pl.BlockSpec(memory_space=pl.ANY)] * 5,
        out_specs=pl.BlockSpec(memory_space=pltpu.VMEM),
        scratch_shapes=[
            pltpu.VMEM((tokens, width), features.dtype),
            pltpu.VMEM((tokens, heads, top), jnp.int32),
            pltpu.VMEM((tokens, heads, top), jnp.float32),
            pltpu.VMEM((table_rows, width), key_table.dtype),
            pltpu.VMEM((table_rows, width), value_table.dtype),
            pltpu.VMEM((table_rows // LANES * tokens, LANES), jnp.float32),
            pltpu.VMEM(packed_shape, jnp.int32),
            pltpu.VMEM((tp_size,) + packed_shape, jnp.float32),
            pltpu.VMEM(packed_shape, jnp.float32),
            pltpu.VMEM((tokens, width), jnp.float32),
            pltpu.VMEM((ep_size - 1, own_tokens, width), jnp.float32),
            dma((5,)),
            dma((3, ep_size - 1)),
            dma((3, ep_size - 1)),
            dma((tp_size - 1,)),
            dma((tp_size - 1,)),
            dma((ep_size - 1,)),
            dma((ep_size - 1,)),
        ],
        compiler_params=pltpu.CompilerParams(collective_id=0, has_side_effects=True),
    )(features, key_table, value_table, chosen, scores)


def solution(mesh):
    return jax.shard_map(
        functools.partial(shards, mesh.shape["ep"], mesh.shape["tp"]),
        mesh=mesh,
        in_specs=(
            P("ep", "tp"),
            P("ep", "tp"),
            P("ep", "tp"),
            P("ep", None, None),
            P("ep", None, None),
        ),
        out_specs=P("ep", "tp"),
        check_vma=False,
    )
```

```python
import functools

import jax
import jax.numpy as jnp
from jax import lax
from jax.experimental import pallas as pl
from jax.experimental.pallas import tpu as pltpu
from jax.sharding import PartitionSpec as P

LANES = 128
GROUP = 16
PITCH_PAD = 4
MESH = pl.DeviceIdType.MESH


def matmul_nt(left, right):
    return lax.dot_general(
        left, right, (((1,), (1,)), ((), ())), preferred_element_type=jnp.float32
    )


def split_terms(value):
    upper = value.astype(jnp.bfloat16)
    lower = (value - upper.astype(jnp.float32)).astype(jnp.bfloat16)
    return upper, lower


def kernel(
    ep_size,
    tp_size,
    features_hbm,
    key_hbm,
    value_hbm,
    chosen_hbm,
    scores_hbm,
    out_ref,
    features,
    chosen,
    scores,
    key,
    value,
    dense,
    picks,
    partial,
    weights,
    summed,
    landed,
    local_sem,
    send_sem,
    recv_sem,
    tp_send,
    tp_recv,
    out_send,
    out_recv,
):
    my_ep = lax.axis_index("ep")
    my_tp = lax.axis_index("tp")
    table_rows = key.shape[0]
    blocks = table_rows // LANES
    own_tokens, heads, top = chosen_hbm.shape
    tokens = ep_size * own_tokens
    half = tokens // 2
    pitch = tokens + PITCH_PAD
    per_token = heads * top
    width = 2 * per_token

    def token_slot(ref, index):
        return ref.at[pl.ds(index * own_tokens, own_tokens)]

    small = (
        (features_hbm, features),
        (chosen_hbm, chosen),
        (scores_hbm, scores),
    )
    small_copies = []
    for number, (source, target) in enumerate(small):
        copy = pltpu.make_async_copy(source, token_slot(target, my_ep), local_sem.at[number])
        copy.start()
        small_copies.append(copy)
    key_copy = pltpu.make_async_copy(key_hbm, key, local_sem.at[3])
    key_copy.start()
    value_copy = pltpu.make_async_copy(value_hbm, value, local_sem.at[4])
    value_copy.start()

    barrier = pltpu.get_barrier_semaphore()
    for step in range(1, ep_size):
        pl.semaphore_signal(
            barrier, inc=1, device_id=(lax.rem(my_ep + step, ep_size), my_tp), device_id_type=MESH
        )
    for step in range(1, tp_size):
        pl.semaphore_signal(
            barrier, inc=1, device_id=(my_ep, lax.rem(my_tp + step, tp_size)), device_id_type=MESH
        )
    for copy in small_copies:
        copy.wait()
    pl.semaphore_wait(barrier, ep_size + tp_size - 2)

    def ep_copy(number, step, owner):
        target = small[number][1]
        return pltpu.make_async_remote_copy(
            src_ref=token_slot(target, owner),
            dst_ref=token_slot(target, owner),
            send_sem=send_sem.at[number, step - 1],
            recv_sem=recv_sem.at[number, step - 1],
            device_id=(lax.rem(my_ep + step, ep_size), my_tp),
            device_id_type=MESH,
        )

    def source_ep(step):
        return lax.rem(my_ep + ep_size - step, ep_size)

    for number in range(3):
        for step in range(1, ep_size):
            ep_copy(number, step, my_ep).start()

    for step in range(1, ep_size):
        ep_copy(0, step, source_ep(step)).wait_recv()
    key_copy.wait()

    token_vectors = features[...]

    def dense_step(index, carry):
        for inner in range(GROUP):
            block = index * GROUP + inner
            rows = key[pl.ds(pl.multiple_of(block * LANES, LANES), LANES), :]
            dense[pl.ds(block * pitch, tokens), :] = matmul_nt(
                token_vectors, rows
            )
        return carry

    lax.fori_loop(0, blocks // GROUP, dense_step, 0)

    for step in range(1, ep_size):
        ep_copy(1, step, source_ep(step)).wait_recv()

    def packed(pieces):
        flat = jnp.concatenate(pieces, axis=1)
        return jnp.concatenate([flat[:half], flat[half:]], axis=1)

    picks[...] = packed([chosen[:, head, :] for head in range(heads)]) - my_ep * table_rows

    block_ids = lax.broadcasted_iota(jnp.int32, (blocks, width), 0)
    lane_ids = lax.broadcasted_iota(jnp.int32, (LANES, width), 0)
    in_first = lax.broadcasted_iota(jnp.int32, (blocks, width), 1) < per_token

    def masks(pair):
        row = picks[pl.ds(pair, 1), :]
        column_hot = jnp.where((row & (LANES - 1)) == lane_ids, 1.0, 0.0).astype(jnp.bfloat16)
        block_mask = lax.shift_right_arithmetic(row, 7) == block_ids
        return column_hot, block_mask

    def chosen_of(token, column_hot):
        upper, lower = split_terms(dense[pl.ds(token, blocks, stride=pitch), :])
        return jnp.dot(upper, column_hot, preferred_element_type=jnp.float32) + jnp.dot(
            lower, column_hot, preferred_element_type=jnp.float32
        )

    def pick_step(pair, carry):
        column_hot, block_mask = masks(pair)
        both = jnp.where(
            in_first, chosen_of(pair, column_hot), chosen_of(pair + half, column_hot)
        )
        partial[my_tp, pl.ds(pair, 1), :] = jnp.sum(
            jnp.where(block_mask, both, 0.0), axis=0, keepdims=True
        )
        return carry

    lax.fori_loop(0, half, pick_step, 0, unroll=2)

    def tp_copy(step, owner):
        return pltpu.make_async_remote_copy(
            src_ref=partial.at[owner],
            dst_ref=partial.at[owner],
            send_sem=tp_send.at[step - 1],
            recv_sem=tp_recv.at[step - 1],
            device_id=(my_ep, lax.rem(my_tp + step, tp_size)),
            device_id_type=MESH,
        )

    for step in range(1, tp_size):
        tp_copy(step, my_tp).start()

    for step in range(1, ep_size):
        ep_copy(2, step, source_ep(step)).wait_recv()
    gate_pieces = []
    for head in range(heads):
        logits = scores[:, head, :]
        powers = jnp.exp(logits - jnp.max(logits, axis=1, keepdims=True))
        gate_pieces.append(powers / jnp.sum(powers, axis=1, keepdims=True))
    gates = packed(gate_pieces)

    for step in range(1, tp_size):
        tp_copy(step, lax.rem(my_tp + tp_size - step, tp_size)).wait_recv()
    products = partial[0]
    for index in range(1, tp_size):
        products = products + partial[index]
    activated = 0.5 * products * (1.0 + lax.erf(products * (0.5**0.5)))
    weights[...] = (gates * activated).astype(jnp.bfloat16).astype(jnp.float32)

    def spread_step(pair, carry):
        column_hot, block_mask = masks(pair)
        hot = jnp.where(block_mask, weights[pl.ds(pair, 1), :], 0.0)
        for token, keep in ((pair, in_first), (pair + half, jnp.logical_not(in_first))):
            dense[pl.ds(token, blocks, stride=pitch), :] = matmul_nt(
                jnp.where(keep, hot, 0.0).astype(jnp.bfloat16), column_hot
            )
        return carry

    lax.fori_loop(0, half, spread_step, 0, unroll=2)

    value_copy.wait()

    def value_step(index, total):
        for inner in range(GROUP):
            block = index * GROUP + inner
            rows = value[pl.ds(pl.multiple_of(block * LANES, LANES), LANES), :]
            upper, lower = split_terms(
                dense[pl.ds(block * pitch, tokens), :]
            )
            both = jnp.concatenate([upper, lower], axis=0)
            total = total + jnp.dot(both, rows, preferred_element_type=jnp.float32)
        return total

    zero = jnp.zeros((2 * tokens, summed.shape[1]), jnp.float32)
    total = lax.fori_loop(0, blocks // GROUP, value_step, zero)
    summed[...] = total[:tokens] + total[tokens:]

    def out_copy(step, owner):
        return pltpu.make_async_remote_copy(
            src_ref=token_slot(summed, lax.rem(my_ep + step, ep_size)),
            dst_ref=landed.at[step - 1],
            send_sem=out_send.at[step - 1],
            recv_sem=out_recv.at[step - 1],
            device_id=(lax.rem(my_ep + step, ep_size), my_tp),
            device_id_type=MESH,
        )

    for step in range(1, ep_size):
        out_copy(step, my_ep).start()
    result = summed[pl.ds(pl.multiple_of(my_ep * own_tokens, own_tokens), own_tokens), :]
    for step in range(1, ep_size):
        out_copy(step, my_ep).wait_recv()
        result = result + landed[step - 1]
    out_ref[...] = result.astype(out_ref.dtype)

    for step in range(1, ep_size):
        for number in range(3):
            ep_copy(number, step, my_ep).wait_send()
        out_copy(step, my_ep).wait_send()
    for step in range(1, tp_size):
        tp_copy(step, my_tp).wait_send()


def shards(ep_size, tp_size, features, key_table, value_table, chosen, scores):
    own_tokens, width = features.shape
    _, heads, top = chosen.shape
    table_rows = key_table.shape[0]
    tokens = ep_size * own_tokens
    packed_shape = (tokens // 2, 2 * heads * top)
    dma = pltpu.SemaphoreType.DMA
    return pl.pallas_call(
        functools.partial(kernel, ep_size, tp_size),
        out_shape=jax.ShapeDtypeStruct((own_tokens, width), jnp.bfloat16),
        in_specs=[pl.BlockSpec(memory_space=pl.ANY)] * 5,
        out_specs=pl.BlockSpec(memory_space=pltpu.VMEM),
        scratch_shapes=[
            pltpu.VMEM((tokens, width), features.dtype),
            pltpu.VMEM((tokens, heads, top), jnp.int32),
            pltpu.VMEM((tokens, heads, top), jnp.float32),
            pltpu.VMEM((table_rows, width), key_table.dtype),
            pltpu.VMEM((table_rows, width), value_table.dtype),
            pltpu.VMEM((table_rows // LANES * (tokens + PITCH_PAD), LANES), jnp.float32),
            pltpu.VMEM(packed_shape, jnp.int32),
            pltpu.VMEM((tp_size,) + packed_shape, jnp.float32),
            pltpu.VMEM(packed_shape, jnp.float32),
            pltpu.VMEM((tokens, width), jnp.float32),
            pltpu.VMEM((ep_size - 1, own_tokens, width), jnp.float32),
            dma((5,)),
            dma((3, ep_size - 1)),
            dma((3, ep_size - 1)),
            dma((tp_size - 1,)),
            dma((tp_size - 1,)),
            dma((ep_size - 1,)),
            dma((ep_size - 1,)),
        ],
        compiler_params=pltpu.CompilerParams(collective_id=0, has_side_effects=True),
    )(features, key_table, value_table, chosen, scores)


def solution(mesh):
    return jax.shard_map(
        functools.partial(shards, mesh.shape["ep"], mesh.shape["tp"]),
        mesh=mesh,
        in_specs=(
            P("ep", "tp"),
            P("ep", "tp"),
            P("ep", "tp"),
            P("ep", None, None),
            P("ep", None, None),
        ),
        out_specs=P("ep", "tp"),
        check_vma=False,
    )
```

```python
import functools

import jax
import jax.numpy as jnp
from jax import lax
from jax.experimental import pallas as pl
from jax.experimental.pallas import tpu as pltpu
from jax.sharding import PartitionSpec as P

LANES = 128
GROUP = 64
PITCH_PAD = 4
MESH = pl.DeviceIdType.MESH


def matmul_nt(left, right):
    return lax.dot_general(
        left, right, (((1,), (1,)), ((), ())), preferred_element_type=jnp.float32
    )


def split_terms(value):
    upper = value.astype(jnp.bfloat16)
    lower = (value - upper.astype(jnp.float32)).astype(jnp.bfloat16)
    return upper, lower


def kernel(
    ep_size,
    tp_size,
    features_hbm,
    key_hbm,
    value_hbm,
    chosen_hbm,
    scores_hbm,
    out_ref,
    features,
    chosen,
    scores,
    picks,
    gates,
    key,
    value,
    dense,
    partial,
    weights,
    summed,
    landed,
    local_sem,
    send_sem,
    recv_sem,
    tp_send,
    tp_recv,
    out_send,
    out_recv,
):
    my_ep = lax.axis_index("ep")
    my_tp = lax.axis_index("tp")
    table_rows = key.shape[0]
    blocks = table_rows // LANES
    own_tokens, heads, top = chosen_hbm.shape
    tokens = ep_size * own_tokens
    own_pairs = own_tokens // 2
    pitch = tokens + PITCH_PAD
    per_token = heads * top
    width = 2 * per_token

    def token_slot(ref, index):
        return ref.at[pl.ds(index * own_tokens, own_tokens)]

    def pair_slot(ref, index):
        return ref.at[pl.ds(pl.multiple_of(index * own_pairs, own_pairs), own_pairs)]

    small = (
        (features_hbm, token_slot(features, my_ep)),
        (chosen_hbm, chosen),
        (scores_hbm, scores),
    )
    small_copies = []
    for number, (source, target) in enumerate(small):
        copy = pltpu.make_async_copy(source, target, local_sem.at[number])
        copy.start()
        small_copies.append(copy)
    key_copy = pltpu.make_async_copy(key_hbm, key, local_sem.at[3])
    key_copy.start()
    value_copy = pltpu.make_async_copy(value_hbm, value, local_sem.at[4])
    value_copy.start()

    barrier = pltpu.get_barrier_semaphore()
    for step in range(1, ep_size):
        pl.semaphore_signal(
            barrier, inc=1, device_id=(lax.rem(my_ep + step, ep_size), my_tp), device_id_type=MESH
        )
    for step in range(1, tp_size):
        pl.semaphore_signal(
            barrier, inc=1, device_id=(my_ep, lax.rem(my_tp + step, tp_size)), device_id_type=MESH
        )
    for copy in small_copies:
        copy.wait()

    def packed(pieces):
        flat = jnp.concatenate(pieces, axis=1)
        return jnp.concatenate([flat[:own_pairs], flat[own_pairs:]], axis=1)

    pair_slot(picks, my_ep)[...] = packed([chosen[:, head, :] for head in range(heads)])
    gate_pieces = []
    for head in range(heads):
        logits = scores[:, head, :]
        powers = jnp.exp(logits - jnp.max(logits, axis=1, keepdims=True))
        gate_pieces.append(powers / jnp.sum(powers, axis=1, keepdims=True))
    pair_slot(gates, my_ep)[...] = packed(gate_pieces)
    pl.semaphore_wait(barrier, ep_size + tp_size - 2)

    def ep_copy(number, step, owner):
        slot = (
            token_slot(features, owner),
            pair_slot(picks, owner),
            pair_slot(gates, owner),
        )[number]
        return pltpu.make_async_remote_copy(
            src_ref=slot,
            dst_ref=slot,
            send_sem=send_sem.at[number, step - 1],
            recv_sem=recv_sem.at[number, step - 1],
            device_id=(lax.rem(my_ep + step, ep_size), my_tp),
            device_id_type=MESH,
        )

    def source_ep(step):
        return lax.rem(my_ep + ep_size - step, ep_size)

    for number in range(3):
        for step in range(1, ep_size):
            ep_copy(number, step, my_ep).start()

    for step in range(1, ep_size):
        ep_copy(0, step, source_ep(step)).wait_recv()
    key_copy.wait()

    token_vectors = features[...]

    def dense_step(index, carry):
        for inner in range(GROUP):
            block = index * GROUP + inner
            rows = key[pl.ds(pl.multiple_of(block * LANES, LANES), LANES), :]
            dense[pl.ds(block * pitch, tokens), :] = matmul_nt(
                token_vectors, rows
            )
        return carry

    lax.fori_loop(0, blocks // GROUP, dense_step, 0)

    for step in range(1, ep_size):
        ep_copy(1, step, source_ep(step)).wait_recv()

    first_row = my_ep * table_rows
    block_ids = lax.broadcasted_iota(jnp.int32, (blocks, width), 0)
    lane_ids = lax.broadcasted_iota(jnp.int32, (LANES, width), 0)
    in_first = lax.broadcasted_iota(jnp.int32, (blocks, width), 1) < per_token

    def masks(pair):
        row = picks[pl.ds(pair, 1), :] - first_row
        column_hot = jnp.where((row & (LANES - 1)) == lane_ids, 1.0, 0.0).astype(jnp.bfloat16)
        block_mask = lax.shift_right_arithmetic(row, 7) == block_ids
        return column_hot, block_mask

    def chosen_of(token, column_hot):
        upper, lower = split_terms(dense[pl.ds(token, blocks, stride=pitch), :])
        return jnp.dot(upper, column_hot, preferred_element_type=jnp.float32) + jnp.dot(
            lower, column_hot, preferred_element_type=jnp.float32
        )

    def pick_step(owner, carry):
        for inner in range(own_pairs):
            pair = owner * own_pairs + inner
            token = owner * own_tokens + inner
            column_hot, block_mask = masks(pair)
            both = jnp.where(
                in_first,
                chosen_of(token, column_hot),
                chosen_of(token + own_pairs, column_hot),
            )
            partial[my_tp, pl.ds(pair, 1), :] = jnp.sum(
                jnp.where(block_mask, both, 0.0), axis=0, keepdims=True
            )
        return carry

    lax.fori_loop(0, ep_size, pick_step, 0)

    def tp_copy(step, owner):
        return pltpu.make_async_remote_copy(
            src_ref=partial.at[owner],
            dst_ref=partial.at[owner],
            send_sem=tp_send.at[step - 1],
            recv_sem=tp_recv.at[step - 1],
            device_id=(my_ep, lax.rem(my_tp + step, tp_size)),
            device_id_type=MESH,
        )

    for step in range(1, tp_size):
        tp_copy(step, my_tp).start()

    for step in range(1, ep_size):
        ep_copy(2, step, source_ep(step)).wait_recv()
    for step in range(1, tp_size):
        tp_copy(step, lax.rem(my_tp + tp_size - step, tp_size)).wait_recv()
    products = partial[0]
    for index in range(1, tp_size):
        products = products + partial[index]
    activated = 0.5 * products * (1.0 + lax.erf(products * (0.5**0.5)))
    weights[...] = (gates[...] * activated).astype(jnp.bfloat16).astype(jnp.float32)

    def spread_step(owner, carry):
        for inner in range(own_pairs):
            pair = owner * own_pairs + inner
            first = owner * own_tokens + inner
            column_hot, block_mask = masks(pair)
            hot = jnp.where(block_mask, weights[pl.ds(pair, 1), :], 0.0)
            for token, keep in (
                (first, in_first),
                (first + own_pairs, jnp.logical_not(in_first)),
            ):
                dense[pl.ds(token, blocks, stride=pitch), :] = matmul_nt(
                    jnp.where(keep, hot, 0.0).astype(jnp.bfloat16), column_hot
                )
        return carry

    lax.fori_loop(0, ep_size, spread_step, 0)

    value_copy.wait()

    def value_step(index, total):
        for inner in range(GROUP):
            block = index * GROUP + inner
            rows = value[pl.ds(pl.multiple_of(block * LANES, LANES), LANES), :]
            upper, lower = split_terms(
                dense[pl.ds(block * pitch, tokens), :]
            )
            both = jnp.concatenate([upper, lower], axis=0)
            total = total + jnp.dot(both, rows, preferred_element_type=jnp.float32)
        return total

    zero = jnp.zeros((2 * tokens, summed.shape[1]), jnp.float32)
    total = lax.fori_loop(0, blocks // GROUP, value_step, zero)
    summed[...] = total[:tokens] + total[tokens:]

    def out_copy(step, owner):
        return pltpu.make_async_remote_copy(
            src_ref=token_slot(summed, lax.rem(my_ep + step, ep_size)),
            dst_ref=landed.at[step - 1],
            send_sem=out_send.at[step - 1],
            recv_sem=out_recv.at[step - 1],
            device_id=(lax.rem(my_ep + step, ep_size), my_tp),
            device_id_type=MESH,
        )

    for step in range(1, ep_size):
        out_copy(step, my_ep).start()
    result = summed[pl.ds(pl.multiple_of(my_ep * own_tokens, own_tokens), own_tokens), :]
    for step in range(1, ep_size):
        out_copy(step, my_ep).wait_recv()
        result = result + landed[step - 1]
    out_ref[...] = result.astype(out_ref.dtype)

    for step in range(1, ep_size):
        for number in range(3):
            ep_copy(number, step, my_ep).wait_send()
        out_copy(step, my_ep).wait_send()
    for step in range(1, tp_size):
        tp_copy(step, my_tp).wait_send()


def shards(ep_size, tp_size, features, key_table, value_table, chosen, scores):
    own_tokens, width = features.shape
    _, heads, top = chosen.shape
    table_rows = key_table.shape[0]
    tokens = ep_size * own_tokens
    packed_shape = (tokens // 2, 2 * heads * top)
    dma = pltpu.SemaphoreType.DMA
    return pl.pallas_call(
        functools.partial(kernel, ep_size, tp_size),
        out_shape=pltpu.VMEM((own_tokens, width), jnp.bfloat16),
        in_specs=[pl.BlockSpec(memory_space=pl.ANY)] * 5,
        out_specs=pl.BlockSpec(memory_space=pltpu.VMEM),
        scratch_shapes=[
            pltpu.VMEM((tokens, width), features.dtype),
            pltpu.VMEM((own_tokens, heads, top), jnp.int32),
            pltpu.VMEM((own_tokens, heads, top), jnp.float32),
            pltpu.VMEM(packed_shape, jnp.int32),
            pltpu.VMEM(packed_shape, jnp.float32),
            pltpu.VMEM((table_rows, width), key_table.dtype),
            pltpu.VMEM((table_rows, width), value_table.dtype),
            pltpu.VMEM((table_rows // LANES * (tokens + PITCH_PAD), LANES), jnp.float32),
            pltpu.VMEM((tp_size,) + packed_shape, jnp.float32),
            pltpu.VMEM(packed_shape, jnp.float32),
            pltpu.VMEM((tokens, width), jnp.float32),
            pltpu.VMEM((ep_size - 1, own_tokens, width), jnp.float32),
            dma((5,)),
            dma((3, ep_size - 1)),
            dma((3, ep_size - 1)),
            dma((tp_size - 1,)),
            dma((tp_size - 1,)),
            dma((ep_size - 1,)),
            dma((ep_size - 1,)),
        ],
        compiler_params=pltpu.CompilerParams(collective_id=0, has_side_effects=True),
    )(features, key_table, value_table, chosen, scores)


def solution(mesh):
    return jax.shard_map(
        functools.partial(shards, mesh.shape["ep"], mesh.shape["tp"]),
        mesh=mesh,
        in_specs=(
            P("ep", "tp"),
            P("ep", "tp"),
            P("ep", "tp"),
            P("ep", None, None),
            P("ep", None, None),
        ),
        out_specs=P("ep", "tp"),
        check_vma=False,
    )
```

```python
import functools

import jax
import jax.numpy as jnp
from jax import lax
from jax.experimental import pallas as pl
from jax.experimental.pallas import tpu as pltpu
from jax.sharding import PartitionSpec as P

LANES = 128
GROUP = 64
PITCH_PAD = 4
CHUNKS = 4
MESH = pl.DeviceIdType.MESH


def matmul_nt(left, right):
    return lax.dot_general(
        left, right, (((1,), (1,)), ((), ())), preferred_element_type=jnp.float32
    )


def split_terms(value):
    upper = value.astype(jnp.bfloat16)
    lower = (value - upper.astype(jnp.float32)).astype(jnp.bfloat16)
    return upper, lower


def chunk_count(ep_size):
    return CHUNKS if ep_size % CHUNKS == 0 else 1


def kernel(
    ep_size,
    tp_size,
    features_hbm,
    key_hbm,
    value_hbm,
    chosen_hbm,
    scores_hbm,
    out_ref,
    features,
    chosen,
    scores,
    picks,
    gates,
    key,
    key_columns,
    value,
    dense,
    partial,
    weights,
    summed,
    landed,
    local_sem,
    send_sem,
    recv_sem,
    tp_send,
    tp_recv,
    out_send,
    out_recv,
):
    my_ep = lax.axis_index("ep")
    my_tp = lax.axis_index("tp")
    table_rows = key.shape[0]
    blocks = table_rows // LANES
    own_tokens, heads, top = chosen_hbm.shape
    tokens = ep_size * own_tokens
    own_pairs = own_tokens // 2
    chunks = chunk_count(ep_size)
    chunk_owners = ep_size // chunks
    chunk_pairs = chunk_owners * own_pairs
    pitch = tokens + PITCH_PAD
    per_token = heads * top
    width = 2 * per_token

    def token_slot(ref, index):
        return ref.at[pl.ds(index * own_tokens, own_tokens)]

    def pair_slot(ref, index):
        return ref.at[pl.ds(pl.multiple_of(index * own_pairs, own_pairs), own_pairs)]

    small = (
        (features_hbm, token_slot(features, my_ep)),
        (chosen_hbm, chosen),
        (scores_hbm, scores),
    )
    small_copies = []
    for number, (source, target) in enumerate(small):
        copy = pltpu.make_async_copy(source, target, local_sem.at[number])
        copy.start()
        small_copies.append(copy)
    key_copy = pltpu.make_async_copy(key_hbm, key, local_sem.at[3])
    key_copy.start()
    value_copy = pltpu.make_async_copy(value_hbm, value, local_sem.at[4])
    value_copy.start()

    barrier = pltpu.get_barrier_semaphore()
    for step in range(1, ep_size):
        pl.semaphore_signal(
            barrier, inc=1, device_id=(lax.rem(my_ep + step, ep_size), my_tp), device_id_type=MESH
        )
    for step in range(1, tp_size):
        pl.semaphore_signal(
            barrier, inc=1, device_id=(my_ep, lax.rem(my_tp + step, tp_size)), device_id_type=MESH
        )
    for copy in small_copies:
        copy.wait()

    def packed(pieces):
        flat = jnp.concatenate(pieces, axis=1)
        return jnp.concatenate([flat[:own_pairs], flat[own_pairs:]], axis=1)

    pair_slot(picks, my_ep)[...] = packed([chosen[:, head, :] for head in range(heads)])
    gate_pieces = []
    for head in range(heads):
        logits = scores[:, head, :]
        powers = jnp.exp(logits - jnp.max(logits, axis=1, keepdims=True))
        gate_pieces.append(powers / jnp.sum(powers, axis=1, keepdims=True))
    pair_slot(gates, my_ep)[...] = packed(gate_pieces)
    pl.semaphore_wait(barrier, ep_size + tp_size - 2)

    def ep_copy(number, step, owner):
        slot = (
            token_slot(features, owner),
            pair_slot(picks, owner),
            pair_slot(gates, owner),
        )[number]
        return pltpu.make_async_remote_copy(
            src_ref=slot,
            dst_ref=slot,
            send_sem=send_sem.at[number, step - 1],
            recv_sem=recv_sem.at[number, step - 1],
            device_id=(lax.rem(my_ep + step, ep_size), my_tp),
            device_id_type=MESH,
        )

    def source_ep(step):
        return lax.rem(my_ep + ep_size - step, ep_size)

    for number in range(3):
        for step in range(1, ep_size):
            ep_copy(number, step, my_ep).start()

    depth = key.shape[1]

    def turn_step(index, carry):
        for inner in range(GROUP):
            block = index * GROUP + inner
            rows = key[pl.ds(pl.multiple_of(block * LANES, LANES), LANES), :]
            key_columns[pl.ds(pl.multiple_of(block * depth, depth), depth), :] = rows.T
        return carry

    key_copy.wait()
    lax.fori_loop(0, blocks // GROUP, turn_step, 0)

    for step in range(1, ep_size):
        ep_copy(0, step, source_ep(step)).wait_recv()
    token_vectors = features[...]

    def dense_step(index, carry):
        for inner in range(GROUP):
            block = index * GROUP + inner
            columns = key_columns[pl.ds(pl.multiple_of(block * depth, depth), depth), :]
            dense[pl.ds(block * pitch, tokens), :] = jnp.dot(
                token_vectors, columns, preferred_element_type=jnp.float32
            )
        return carry

    lax.fori_loop(0, blocks // GROUP, dense_step, 0)

    for step in range(1, ep_size):
        ep_copy(1, step, source_ep(step)).wait_recv()

    first_row = my_ep * table_rows
    block_ids = lax.broadcasted_iota(jnp.int32, (blocks, width), 0)
    lane_ids = lax.broadcasted_iota(jnp.int32, (LANES, width), 0)
    in_first = lax.broadcasted_iota(jnp.int32, (blocks, width), 1) < per_token

    def masks(pair):
        row = picks[pl.ds(pair, 1), :] - first_row
        column_hot = jnp.where((row & (LANES - 1)) == lane_ids, 1.0, 0.0).astype(jnp.bfloat16)
        block_mask = lax.shift_right_arithmetic(row, 7) == block_ids
        return column_hot, block_mask

    def chosen_of(token, column_hot):
        upper, lower = split_terms(dense[pl.ds(token, blocks, stride=pitch), :])
        return jnp.dot(upper, column_hot, preferred_element_type=jnp.float32) + jnp.dot(
            lower, column_hot, preferred_element_type=jnp.float32
        )

    def chunk_rows(chunk):
        return pl.ds(pl.multiple_of(chunk * chunk_pairs, chunk_pairs), chunk_pairs)

    def tp_copy(step, owner, chunk):
        slot = partial.at[owner, chunk_rows(chunk)]
        return pltpu.make_async_remote_copy(
            src_ref=slot,
            dst_ref=slot,
            send_sem=tp_send.at[step - 1, chunk],
            recv_sem=tp_recv.at[step - 1, chunk],
            device_id=(my_ep, lax.rem(my_tp + step, tp_size)),
            device_id_type=MESH,
        )

    def pick_step(owner, carry):
        for inner in range(own_pairs):
            pair = owner * own_pairs + inner
            token = owner * own_tokens + inner
            column_hot, block_mask = masks(pair)
            both = jnp.where(
                in_first,
                chosen_of(token, column_hot),
                chosen_of(token + own_pairs, column_hot),
            )
            partial[my_tp, pl.ds(pair, 1), :] = jnp.sum(
                jnp.where(block_mask, both, 0.0), axis=0, keepdims=True
            )
        return carry

    def pick_chunk(chunk, carry):
        if chunk_owners == 1:
            pick_step(chunk, 0)
        else:
            first = chunk * chunk_owners
            lax.fori_loop(first, first + chunk_owners, pick_step, 0)
        for step in range(1, tp_size):
            tp_copy(step, my_tp, chunk).start()
        return carry

    lax.fori_loop(0, chunks, pick_chunk, 0)

    for step in range(1, ep_size):
        ep_copy(2, step, source_ep(step)).wait_recv()
    def spread_step(owner, carry):
        for inner in range(own_pairs):
            pair = owner * own_pairs + inner
            first = owner * own_tokens + inner
            column_hot, block_mask = masks(pair)
            hot = jnp.where(block_mask, weights[pl.ds(pair, 1), :], 0.0)
            for token, keep in (
                (first, in_first),
                (first + own_pairs, jnp.logical_not(in_first)),
            ):
                dense[pl.ds(token, blocks, stride=pitch), :] = matmul_nt(
                    jnp.where(keep, hot, 0.0).astype(jnp.bfloat16), column_hot
                )
        return carry

    def spread_chunk(chunk, carry):
        for step in range(1, tp_size):
            tp_copy(step, lax.rem(my_tp + tp_size - step, tp_size), chunk).wait_recv()
        rows = chunk_rows(chunk)
        products = partial[0, rows, :]
        for index in range(1, tp_size):
            products = products + partial[index, rows, :]
        activated = 0.5 * products * (1.0 + lax.erf(products * (0.5**0.5)))
        row_weights = (gates[rows, :] * activated).astype(jnp.bfloat16)
        weights[rows, :] = row_weights.astype(jnp.float32)
        if chunk_owners == 1:
            spread_step(chunk, 0)
        else:
            first = chunk * chunk_owners
            lax.fori_loop(first, first + chunk_owners, spread_step, 0)
        return carry

    lax.fori_loop(0, chunks, spread_chunk, 0)

    value_copy.wait()

    def value_step(index, total):
        for inner in range(GROUP):
            block = index * GROUP + inner
            rows = value[pl.ds(pl.multiple_of(block * LANES, LANES), LANES), :]
            upper, lower = split_terms(
                dense[pl.ds(block * pitch, tokens), :]
            )
            both = jnp.concatenate([upper, lower], axis=0)
            total = total + jnp.dot(both, rows, preferred_element_type=jnp.float32)
        return total

    zero = jnp.zeros((2 * tokens, summed.shape[1]), jnp.float32)
    total = lax.fori_loop(0, blocks // GROUP, value_step, zero)
    summed[...] = total[:tokens] + total[tokens:]

    def out_copy(step, owner):
        return pltpu.make_async_remote_copy(
            src_ref=token_slot(summed, lax.rem(my_ep + step, ep_size)),
            dst_ref=landed.at[step - 1],
            send_sem=out_send.at[step - 1],
            recv_sem=out_recv.at[step - 1],
            device_id=(lax.rem(my_ep + step, ep_size), my_tp),
            device_id_type=MESH,
        )

    for step in range(1, ep_size):
        out_copy(step, my_ep).start()
    result = summed[pl.ds(pl.multiple_of(my_ep * own_tokens, own_tokens), own_tokens), :]
    for step in range(1, ep_size):
        out_copy(step, my_ep).wait_recv()
        result = result + landed[step - 1]
    out_ref[...] = result.astype(out_ref.dtype)

    for step in range(1, ep_size):
        for number in range(3):
            ep_copy(number, step, my_ep).wait_send()
        out_copy(step, my_ep).wait_send()
    for step in range(1, tp_size):
        for chunk in range(chunks):
            tp_copy(step, my_tp, chunk).wait_send()


def shards(ep_size, tp_size, features, key_table, value_table, chosen, scores):
    own_tokens, width = features.shape
    _, heads, top = chosen.shape
    table_rows = key_table.shape[0]
    tokens = ep_size * own_tokens
    packed_shape = (tokens // 2, 2 * heads * top)
    dma = pltpu.SemaphoreType.DMA
    return pl.pallas_call(
        functools.partial(kernel, ep_size, tp_size),
        out_shape=pltpu.VMEM((own_tokens, width), jnp.bfloat16),
        in_specs=[pl.BlockSpec(memory_space=pl.ANY)] * 5,
        out_specs=pl.BlockSpec(memory_space=pltpu.VMEM),
        scratch_shapes=[
            pltpu.VMEM((tokens, width), features.dtype),
            pltpu.VMEM((own_tokens, heads, top), jnp.int32),
            pltpu.VMEM((own_tokens, heads, top), jnp.float32),
            pltpu.VMEM(packed_shape, jnp.int32),
            pltpu.VMEM(packed_shape, jnp.float32),
            pltpu.VMEM((table_rows, width), key_table.dtype),
            pltpu.VMEM((table_rows // LANES * width, LANES), key_table.dtype),
            pltpu.VMEM((table_rows, width), value_table.dtype),
            pltpu.VMEM((table_rows // LANES * (tokens + PITCH_PAD), LANES), jnp.float32),
            pltpu.VMEM((tp_size,) + packed_shape, jnp.float32),
            pltpu.VMEM(packed_shape, jnp.float32),
            pltpu.VMEM((tokens, width), jnp.float32),
            pltpu.VMEM((ep_size - 1, own_tokens, width), jnp.float32),
            dma((5,)),
            dma((3, ep_size - 1)),
            dma((3, ep_size - 1)),
            dma((tp_size - 1, chunk_count(ep_size))),
            dma((tp_size - 1, chunk_count(ep_size))),
            dma((ep_size - 1,)),
            dma((ep_size - 1,)),
        ],
        compiler_params=pltpu.CompilerParams(collective_id=0, has_side_effects=True),
    )(features, key_table, value_table, chosen, scores)


def solution(mesh):
    return jax.shard_map(
        functools.partial(shards, mesh.shape["ep"], mesh.shape["tp"]),
        mesh=mesh,
        in_specs=(
            P("ep", "tp"),
            P("ep", "tp"),
            P("ep", "tp"),
            P("ep", None, None),
            P("ep", None, None),
        ),
        out_specs=P("ep", "tp"),
        check_vma=False,
    )
```
